32 devices in a mesh: grp: 2 (over x), ep: 8 (over z, y), tp: 2 (over core).
Axes of the slice: x: 2, y: 2, z: 4, core: 2. Of those that a mesh axis runs over, the one named last changes fastest.
Arguments:
- tokens: bfloat16 [3072, 2048], P(('grp', 'ep'), 'tp'), parts along dimension 0, may hold values from -10 to 10
- gain_in: float32 [2048], replicated, may hold values from 0.1 to 1.9
- gain_out: float32 [2048], replicated, may hold values from 0.1 to 1.9
- expert_ids: int32 [3072, 2], P(('grp', 'ep')), parts along dimension 0, may hold values from 0 to 3, all different within a row; in each aligned block of 192 rows (0 to 191, 192 to 383, ...) at most 144 rows name the same one
- route_weight: float32 [3072, 2], P(('grp', 'ep')), parts along dimension 0, may hold values from 0.1 to 1
- gate_weight: bfloat16 [8, 2048, 1792], P('ep', None, 'tp'), may hold values from -0.125 to 0.125
- up_weight: bfloat16 [8, 2048, 1792], P('ep', None, 'tp'), may hold values from -0.125 to 0.125
- down_weight: bfloat16 [8, 1792, 2048], P('ep', 'tp'), may hold values from -1 to 1
Outputs:
- layer_out: bfloat16 [3072, 2048], P(('grp', 'ep'), 'tp'), parts along dimension 0
The draws below stay inside these ranges and needn't reach their ends.
There are 2 independent parts, one for each index of `grp`. The reference program is written for one: setup_inputs(seed, part) draws one part's arguments, and reference() takes and returns one part's arrays. A program takes and returns all parts, laid end to end along the dimension named above; an argument that names none is the same for every part. Nothing has to cross between parts.
Inputs may be any that keep to these rules, and one draw needn't show every extreme that they name: `expert_ids`: each row names 2 different experts. Among the tokens of one index of ep no expert is named more than 144 times, a bound that some block reaches.
All inputs are finite; a program needn't handle non-finite values.
Results may differ from the reference program's by a relative error of at most 0.0077.
Values may be sent and summed in bfloat16 or wider, within the bound.
A program may use at most 64 MiB of HBM per device.

```python
import math
import jax
import jax.numpy as jnp
import numpy as np
from jax import lax

D = 2048
DE = 3584
TOP_K = 2
TOK_EP = 192
EXPERTS = 4
TOKENS = 1536
CAP = 144
N_EP = 8


def column_factors(key):
    key_low, key_high, key_flip = jax.random.split(jax.random.fold_in(key, 11), 3)
    lowest = jax.random.uniform(key_low, (), jnp.float32, 0.35, 0.55)
    highest = jax.random.uniform(key_high, (), jnp.float32, 1.7, 2.4)
    flipped = jax.random.randint(key_flip, (), 0, 2) == 1
    first_half = jnp.where(flipped, highest, lowest)
    second_half = jnp.where(flipped, lowest, highest)
    return jnp.concatenate([jnp.full((D // 2,), first_half, jnp.float32), jnp.full((D - D // 2,), second_half, jnp.float32)])


def draw_tokens(key, part):
    key_base, key_rows = jax.random.split(jax.random.fold_in(key, 3))
    base = jnp.clip(jax.random.normal(key_base, (TOKENS, D), jnp.float32), -4.0, 4.0)
    return (base * column_factors(jax.random.fold_in(key, 5))[None, :]).astype(jnp.bfloat16)


def draw_down_weight(key, part):
    key_base = jax.random.fold_in(key, 7)
    base = jnp.clip(jax.random.normal(key_base, (2 * EXPERTS, DE // 2, D), jnp.float32), -4.0, 4.0)
    base = base * DE ** (-0.5)
    return (base * column_factors(jax.random.fold_in(key, 9))[None, None, :]).astype(jnp.bfloat16)


def block_levels(rng, shape, pieces, low, top_value):
    factor_of, own = 1.0, jax.random.fold_in(rng, 6)
    for position, blocks in pieces:
        steps = jnp.exp(jax.random.uniform(jax.random.fold_in(own, position), (blocks,), jnp.float32, low / len(pieces), top_value / len(pieces)))
        factor_of = factor_of * jnp.repeat(steps, shape[position] // blocks).reshape([-1 if axis == position else 1 for axis in range(len(shape))])
    return factor_of


def routed_block(rng, own, number, rows, count, top, bound, slope):
    ranking = jax.random.permutation(rng, count)
    heavy_load, usual = portions_of(count, rows * top, bound, slope, True), portions_of(count, rows * top, bound, slope, False)
    places = jnp.arange(count)

    def named(sizes, offset_by):
        used = int((sizes > 0).sum())
        fixed = max(1, used // 4)
        moved = fixed + (places - fixed + offset_by * (used - fixed)) % max(1, count - fixed)
        return jnp.zeros((count,), jnp.int32).at[ranking[jnp.where(places < fixed, places, moved)]].set(jnp.asarray(sizes, jnp.int32))

    sizes = jnp.where(number % 4 == 0, named(heavy_load, number // 4), named(usual, number - number // 4 - 1))
    mixed = jax.random.permutation(jax.random.fold_in(own, 3), count)
    source_of, sink = mixed[0:count // 2 * 2:2], mixed[1:count // 2 * 2:2]
    room = jnp.minimum(sizes[source_of] - 1, bound - sizes[sink]) // 2
    room = jnp.where((source_of == ranking[0]) | (sink == ranking[0]) | (sizes[sink] == 0), 0, jnp.maximum(room, 0))
    moved = jax.random.randint(jax.random.fold_in(own, 4), (count // 2,), 0, 1 << 20) % (room + 1)
    sizes = sizes.at[source_of].add(-moved).at[sink].add(moved)
    labels = jnp.searchsorted(jnp.cumsum(sizes), jnp.arange(rows * top), side="right").astype(jnp.int32)
    table = labels.reshape(top, rows).T
    table = table[jax.random.permutation(jax.random.fold_in(own, 1), rows)]
    offset_by = jax.random.randint(jax.random.fold_in(own, 2), (rows, 1), 0, top)
    return jnp.take_along_axis(table, (jnp.arange(top)[None, :] + offset_by) % top, axis=1)


def portions_of(amount, total, bound, skew, full):
    weights = [(1 << 20) // math.isqrt(rank ** skew) + 1 for rank in range(1, amount + 1)]
    largest = bound if full else min(bound, max(-(-total // amount), total * weights[0] // sum(weights)))
    least = 1 if total - largest >= amount - 1 else 0
    counts, surplus = [largest] + [least] * (amount - 1), total - largest - least * (amount - 1)
    while surplus > 0:
        free = [i for i in range(1, amount) if counts[i] < largest] or [i for i in range(1, amount) if counts[i] < bound]
        pool, budget = sum([weights[i] for i in free]), surplus
        for i in free:
            more = min(bound - counts[i], max(1, budget * weights[i] // pool), surplus)
            counts[i] = counts[i] + more
            surplus = surplus - more
    return np.array(counts)


def scatter_about(rng, dims, deviation, limit, cuts=(), kind=jnp.bfloat16):
    result = jax.random.normal(rng, dims, jnp.float32) * deviation
    if len(cuts) > 0:
        result = block_levels(rng, dims, cuts, -0.22, 0.18) * result
    return jnp.clip(result, min=-limit, max=limit).astype(kind)


def setup_inputs(seed: int = 0, part: int = 0) -> dict:
    seeds = jax.random.split(jax.random.key(seed), 9)
    own_keys = jax.random.split(jax.random.fold_in(seeds[8], part), 9)
    tokens = draw_tokens(jax.random.fold_in(jax.random.fold_in(seeds[8], part), 71), part)
    gain_in = jnp.clip(1.0 + 0.18 * jax.random.normal(seeds[1], (D,), jnp.float32), 0.1, 1.9)
    gain_out = jnp.clip(1.0 + 0.18 * jax.random.normal(seeds[2], (D,), jnp.float32), 0.1, 1.9)
    expert_ids_keys = jax.random.split(jax.random.fold_in(own_keys[3], 1), TOKENS // TOK_EP)
    expert_ids_turns = jax.random.permutation(jax.random.fold_in(own_keys[3], 3), TOKENS // TOK_EP)
    expert_ids = jax.vmap(lambda own, number: routed_block(jax.random.fold_in(own_keys[3], 2), own, number, TOK_EP, EXPERTS, TOP_K, CAP, 2))(expert_ids_keys, expert_ids_turns).reshape((TOKENS, TOP_K))
    route_weight = jnp.clip(0.1 + 0.9 * jax.random.uniform(own_keys[4], (TOKENS, TOP_K), jnp.float32) ** block_levels(own_keys[4], (TOKENS, TOP_K), ((0, 8),), -0.2, 0.2), 0.1, 1.0)
    gate_weight = scatter_about(seeds[5], (2 * EXPERTS, D, DE // 2), D ** -0.5, 0.125, ((0, 8), (2, 2)))
    up_weight = scatter_about(seeds[6], (2 * EXPERTS, D, DE // 2), D ** -0.5, 0.125, ((0, 8), (2, 2)))
    down_weight = draw_down_weight(jax.random.fold_in(seeds[8], 71), part)
    return dict(tokens=tokens, gain_in=gain_in, gain_out=gain_out, expert_ids=expert_ids, route_weight=route_weight, gate_weight=gate_weight, up_weight=up_weight, down_weight=down_weight)


norm_eps = 1e-06

def expert_rows(items):
    gathered, gate_pair, up_pair, down_pair = items
    quarter = gate_pair.shape[2] // 2
    rows_float = gathered.astype(jnp.float32)
    total = jnp.zeros((gathered.shape[0], down_pair.shape[2]), jnp.float32)
    for which_half in range(2):
        summed = jnp.zeros((gathered.shape[0], down_pair.shape[2]), jnp.float32)
        for which_core in range(2):
            start_col = which_core * quarter
            gate_pre = jnp.dot(rows_float, gate_pair[which_half, :, start_col:start_col + quarter].astype(jnp.float32), precision=lax.Precision.HIGHEST)
            up_pre = jnp.dot(rows_float, up_pair[which_half, :, start_col:start_col + quarter].astype(jnp.float32), precision=lax.Precision.HIGHEST)
            hidden = (jax.nn.silu(gate_pre) * up_pre).astype(jnp.bfloat16)
            partial_value = jnp.dot(hidden.astype(jnp.float32), down_pair[which_half, start_col:start_col + quarter, :].astype(jnp.float32), precision=lax.Precision.HIGHEST)
            partial_value = lax.optimization_barrier(partial_value.astype(jnp.bfloat16)).astype(jnp.float32)
            summed = summed + partial_value
        total = total + lax.optimization_barrier(summed.astype(jnp.bfloat16)).astype(jnp.float32)
    return total

def reference(tokens, gain_in, gain_out, expert_ids, route_weight, gate_weight, up_weight, down_weight):
    xfloat = tokens.astype(jnp.float32)
    factor = lax.rsqrt(lax.optimization_barrier(jnp.mean(xfloat * xfloat, axis=1, keepdims=True)) + norm_eps)
    normed = (xfloat * factor * gain_in).astype(jnp.bfloat16)
    copies = TOK_EP * TOP_K
    flat_ids = expert_ids.reshape(N_EP, copies).astype(jnp.int32)
    onehot = (flat_ids[:, :, None] == jnp.arange(EXPERTS, dtype=jnp.int32)[None, None, :]).astype(jnp.int32)
    before = jnp.cumsum(onehot, axis=1) - onehot
    slots = lax.optimization_barrier(jnp.sum(before * onehot, axis=2)).astype(jnp.int32)
    targets = (flat_ids * CAP + slots).astype(jnp.int32)
    source = (jnp.arange(copies, dtype=jnp.int32) // TOP_K).astype(jnp.int32)
    blocks = normed.reshape(N_EP, TOK_EP, D)

    def fill(target_rows, block):
        return jnp.zeros((EXPERTS * CAP, D), jnp.bfloat16).at[target_rows].set(block[source])
    buffers = jax.vmap(fill)(targets, blocks)
    per_expert = buffers.reshape(N_EP, EXPERTS, CAP, D).transpose(1, 0, 2, 3).reshape(EXPERTS, N_EP * CAP, D)
    gates = gate_weight.reshape(EXPERTS, 2, D, DE // 2)
    ups = up_weight.reshape(EXPERTS, 2, D, DE // 2)
    downs = down_weight.reshape(EXPERTS, 2, DE // 2, D)
    results = lax.map(expert_rows, (per_expert, gates, ups, downs))
    by_source = results.reshape(EXPERTS, N_EP, CAP, D).transpose(1, 0, 2, 3).reshape(N_EP, EXPERTS * CAP, D)

    def pick(out_rows, target_rows):
        return out_rows[target_rows]
    picked = jax.vmap(pick)(by_source, targets).reshape(TOKENS, TOP_K, D)
    routed = lax.optimization_barrier(jnp.sum(picked * route_weight[:, :, None], axis=1))
    factor_out = lax.rsqrt(lax.optimization_barrier(jnp.mean(routed * routed, axis=1, keepdims=True)) + norm_eps)
    return (routed * factor_out * gain_out).astype(jnp.bfloat16)
```

```python
import functools

import jax
import jax.numpy as jnp
from jax import lax
from jax.experimental import pallas as pl
from jax.experimental.pallas import tpu as pltpu
from jax.sharding import PartitionSpec as P

norm_eps = 1e-06


def plain(
    tokens, gain_in, gain_out, expert_ids, route_weight, gate_weight, up_weight, down_weight
):
    tok_rows, half_width = tokens.shape
    full_width = 2 * half_width
    expert_count = lax.axis_size("ep") // 2
    picks = expert_ids.shape[1]
    capacity = tok_rows * picks * 3 // (2 * expert_count)
    own_cols = lax.axis_index("tp") * half_width
    own_float = tokens.astype(jnp.float32)
    squares = lax.psum(jnp.sum(own_float * own_float, axis=1), "tp")
    factor = lax.rsqrt(squares / full_width + norm_eps)[:, None]
    own_gain = lax.dynamic_slice_in_dim(gain_in, own_cols, half_width)
    normed = (own_float * factor * own_gain).astype(jnp.bfloat16)
    sent_width = normed.shape[1]
    flat_ids = expert_ids.reshape(-1)
    onehot = (flat_ids[:, None] == jnp.arange(expert_count, dtype=jnp.int32)[None, :]).astype(
        jnp.int32
    )
    before = jnp.cumsum(onehot, axis=0) - onehot
    targets = flat_ids * capacity + jnp.sum(before * onehot, axis=1)
    per_token = targets.reshape(tok_rows, picks)
    slot_rows = jnp.arange(expert_count * capacity, dtype=jnp.int32)[:, None]
    placing = jnp.zeros((expert_count * capacity, tok_rows), jnp.bfloat16)
    for which in range(picks):
        placing = placing + (slot_rows == per_token[None, :, which]).astype(jnp.bfloat16)
    packed = jnp.dot(placing, normed, preferred_element_type=jnp.float32).astype(jnp.bfloat16)
    stacked = packed.reshape(expert_count, 1, capacity, sent_width)
    outgoing = jnp.broadcast_to(stacked, (expert_count, 2, capacity, sent_width)).reshape(
        2 * expert_count, capacity, sent_width
    )
    arrived = lax.all_to_all(outgoing, "ep", split_axis=0, concat_axis=0, tiled=True)
    arrived = lax.all_gather(arrived, "tp", axis=2, tiled=True)
    sources = arrived.shape[0]
    gathered = arrived.reshape(sources * capacity, full_width)
    gate_pre = jnp.dot(gathered, gate_weight[0], preferred_element_type=jnp.float32)
    up_pre = jnp.dot(gathered, up_weight[0], preferred_element_type=jnp.float32)
    hidden = (jax.nn.silu(gate_pre) * up_pre).astype(jnp.bfloat16)
    partial_value = jnp.dot(hidden, down_weight[0], preferred_element_type=jnp.float32).astype(
        jnp.bfloat16
    )
    partial_value = partial_value.reshape(sources, capacity, full_width)
    half_sum = lax.psum_scatter(partial_value, "tp", scatter_dimension=2, tiled=True).astype(
        jnp.float32
    )
    returned = lax.all_to_all(
        half_sum.astype(jnp.bfloat16), "ep", split_axis=0, concat_axis=0, tiled=True
    )
    merged = jnp.sum(
        returned.reshape(expert_count, 2, capacity, half_width).astype(jnp.float32), axis=1
    )
    merged = merged.reshape(expert_count * capacity, half_width)
    picked = jnp.take(merged, targets, axis=0).reshape(tok_rows, picks, half_width)
    routed = jnp.sum(picked * route_weight[:, :, None], axis=1)
    squares_out = lax.psum(jnp.sum(routed * routed, axis=1), "tp")
    factor_out = lax.rsqrt(squares_out / full_width + norm_eps)[:, None]
    own_gain_out = lax.dynamic_slice_in_dim(gain_out, own_cols, half_width)
    return (routed * factor_out * own_gain_out).astype(jnp.bfloat16)


MESH = pl.DeviceIdType.MESH


def fused(
    experts,
    cap,
    tok_ref,
    gain_in_ref,
    gain_out_ref,
    ids_ref,
    route_ref,
    gate_hbm,
    up_hbm,
    down_hbm,
    out_ref,
    arrived,
    notes,
    rows,
    parts,
    peer_parts,
    crossing,
    crossed,
    leaving,
    home,
    gate_up,
    down,
    squared,
    peer_squared,
    sums,
    peer_sums,
    total,
    w_sem,
    sq_send,
    sq_recv,
    own_send,
    own_note_send,
    note_send,
    note_recv,
    line_send,
    line_recv,
    core_send,
    core_recv,
    pair_send,
    pair_recv,
    relay_send,
    relay_recv,
    part_send,
    part_recv,
    cross_send,
    cross_recv,
    home_send,
    home_recv,
):
    tok_rows, width = tok_ref.shape
    hidden_width = down.shape[0]
    place = lax.axis_index("ep")
    core = lax.axis_index("tp")
    half = place % 2
    mine = place // 2
    partner = place + 1 - 2 * half
    other = 1 - core
    own_cols = pl.ds(pl.multiple_of(core * width, 128), width)
    other_cols = pl.ds(pl.multiple_of(other * width, 128), width)

    size = ((cap // 16 + 1) // 2 * 16, cap // 16 // 2 * 16)
    begin = (0, size[0])

    def unit(h):
        return pl.ds(begin[h], size[h])

    def side_unit(h, which):
        return pl.ds(2 * begin[h] + which * size[h], size[h])

    def both(h):
        return pl.ds(2 * begin[h], 2 * size[h])

    piece = width // 2

    def cut(p):
        return pl.ds(p * piece, piece)

    def of_core(which, p):
        return pl.ds(pl.multiple_of(which * width + p * piece, 128), piece)

    def turn(where):
        return 1 - 2 * ((2 * where) // experts)

    at_end = (mine == 0) | (mine == experts - 1)
    inner = jnp.logical_not(at_end)

    def at_step(step):
        far = jnp.where(step == 2, experts - 1, jnp.where(step > 2, step - 1, step))
        count = jnp.where(inner, far, step)
        return (mine + turn(mine) * count + experts) % experts

    def on_line(there):
        return {"ep": 2 * there + half}

    loads = [
        pltpu.make_async_copy(gate_hbm.at[0], gate_up.at[:, pl.ds(0, hidden_width)], w_sem.at[0]),
        pltpu.make_async_copy(
            up_hbm.at[0], gate_up.at[:, pl.ds(hidden_width, hidden_width)], w_sem.at[1]
        ),
        pltpu.make_async_copy(down_hbm.at[0], down, w_sem.at[2]),
    ]
    barrier = pltpu.get_barrier_semaphore()
    sides = (-1, 1)

    def inside(where):
        return (where >= 0) & (where < experts)

    def greet(side):
        there = on_line(mine + side)
        pl.semaphore_signal(barrier, inc=1, device_id=there, device_id_type=MESH)

    for side in sides:
        pl.when(inside(mine + side))(functools.partial(greet, side))
    pl.semaphore_signal(barrier, inc=1, device_id={"ep": partner}, device_id_type=MESH)
    pl.semaphore_signal(barrier, inc=1, device_id={"tp": other}, device_id_type=MESH)
    for load in loads:
        load.start()

    def remote(source, target, send, recv, device):
        return pltpu.make_async_remote_copy(
            src_ref=source,
            dst_ref=target,
            send_sem=send,
            recv_sem=recv,
            device_id=device,
            device_id_type=MESH,
        )

    def square_copy():
        return remote(squared, peer_squared, sq_send.at[0], sq_recv.at[0], {"tp": other})

    def sum_copy():
        return remote(sums, peer_sums, sq_send.at[1], sq_recv.at[1], {"tp": other})

    def own_copy(side, p):
        return remote(
            tok_ref.at[:, cut(p)],
            arrived.at[mine, :, cut(p)],
            own_send.at[side + 1 + p],
            line_recv.at[2 * mine + p],
            on_line(mine + side),
        )

    def own_note(side):
        return remote(
            notes.at[mine],
            notes.at[mine],
            own_note_send.at[(side + 1) // 2],
            note_recv.at[mine],
            on_line(mine + side),
        )

    def line_copy(source, p, there):
        view, sem = arrived.at[source, :, cut(p)], 2 * source + p
        return remote(view, view, line_send.at[sem], line_recv.at[sem], on_line(there))

    def note_copy(source, there):
        view = notes.at[source]
        return remote(view, view, note_send.at[source], note_recv.at[source], on_line(there))

    def core_copy(d, p, which):
        view, sem = rows.at[d, 0, :, of_core(which, p)], 2 * d + p
        return remote(view, view, core_send.at[sem], core_recv.at[sem], {"tp": other})

    def pair_copy(d, p):
        return remote(
            rows.at[d, 0, :, of_core(core, p)],
            rows.at[d, 1, :, of_core(core, p)],
            pair_send.at[2 * d + p],
            pair_recv.at[2 * d + p],
            {"ep": partner},
        )

    def relay_copy(d, p, which):
        view, sem = rows.at[d, 1, :, of_core(which, p)], 2 * d + p
        return remote(view, view, relay_send.at[sem], relay_recv.at[sem], {"tp": other})

    def part_copy(d, h):
        return remote(
            parts.at[d, both(h), other_cols],
            peer_parts.at[d, both(h)],
            part_send.at[2 * d + h],
            part_recv.at[2 * d + h],
            {"tp": other},
        )

    def cross_copy(d, h):
        return remote(
            crossing.at[d, unit(h)],
            crossed.at[d, unit(h)],
            cross_send.at[2 * d + h],
            cross_recv.at[2 * d + h],
            {"ep": partner},
        )

    def home_copy(d, h):
        return remote(
            leaving.at[d, unit(h)],
            home.at[mine, unit(h)],
            home_send.at[2 * d + h],
            home_recv.at[2 * mine + h],
            on_line(d),
        )

    def home_arrival(expert, h):
        view, sem = home.at[expert, unit(h)], 2 * expert + h
        return remote(view, view, home_send.at[sem], home_recv.at[sem], on_line(expert))

    own_float = tok_ref[...].astype(jnp.float32)
    squares = jnp.broadcast_to(
        jnp.sum(own_float * own_float, axis=1, keepdims=True), (tok_rows, 128)
    )
    squared[...] = squares.T[0:8, :]
    lead = max(8, experts)
    names = lax.broadcasted_iota(jnp.int32, (lead, tok_rows), 0)
    first = names == ids_ref[0:1, :]
    second = names == ids_ref[1:2, :]
    either = (first.astype(jnp.float32) + second.astype(jnp.float32)).astype(jnp.bfloat16)
    earlier = (
        lax.broadcasted_iota(jnp.int32, (tok_rows, tok_rows), 0)
        < lax.broadcasted_iota(jnp.int32, (tok_rows, tok_rows), 1)
    ).astype(jnp.float32).astype(jnp.bfloat16)
    before = jnp.dot(either, earlier, preferred_element_type=jnp.float32)
    slot_one = jnp.sum(jnp.where(first, before, 0.0), axis=0, keepdims=True).astype(jnp.int32)
    slot_two = jnp.sum(jnp.where(second, before, 0.0), axis=0, keepdims=True).astype(jnp.int32)
    target_one = (ids_ref[0:1, :] * cap + slot_one).astype(jnp.float32)
    target_two = (ids_ref[1:2, :] * cap + slot_two).astype(jnp.float32)

    def slots(expert, first_row, count):
        names = lax.broadcasted_iota(jnp.int32, (count, tok_rows), 0) + expert * cap + first_row
        return names.astype(jnp.float32)

    with jax.named_scope("barrier"):
        pl.semaphore_wait(
            barrier, 2 + (mine > 0).astype(jnp.int32) + (mine < experts - 1).astype(jnp.int32)
        )
    square_copy().start()

    def own_out(side, p):
        own_copy(side, p).start()

    def own_note_out(side):
        own_note(side).start()

    for side in sides:
        pl.when(inside(mine + side))(functools.partial(own_out, side, 0))
    with jax.named_scope("sum0"):
        square_copy().wait_recv()
    factor = lax.rsqrt((squared[...] + peer_squared[...]) / (2 * width) + norm_eps)
    row = lax.broadcasted_iota(jnp.int32, (8, tok_rows), 0)
    notes[mine] = jnp.where(row == 0, target_one, jnp.where(row == 1, target_two, factor))
    for side in sides:
        pl.when(inside(mine + side))(functools.partial(own_note_out, side))
    for side in sides:
        pl.when(inside(mine + side))(functools.partial(own_out, side, 1))

    def fill(source, p, tokens):
        one, two, scale = (notes[source, i : i + 1, :] for i in range(3))
        names = slots(mine, 0, cap)
        placing = jnp.where((names == one) | (names == two), scale, 0.0)
        high = placing.astype(jnp.bfloat16)
        low = (placing - high.astype(jnp.float32)).astype(jnp.bfloat16)
        values = jnp.dot(high, tokens, preferred_element_type=jnp.float32) + jnp.dot(
            low, tokens, preferred_element_type=jnp.float32
        )
        rows[source, 0, :, of_core(core, p)] = (
            values * gain_in_ref[:, of_core(core, p)]
        ).astype(jnp.bfloat16)
        pair_copy(source, p).start()
        core_copy(source, p, core).start()

    def fill_step(step, p):
        source = at_step(step)
        fill(source, p, arrived[source, :, cut(p)])

    def pass_on(step, side, p):
        source, there = mine + side * step, mine - side
        with jax.named_scope("linewait"):
            line_copy(source, p, mine).wait_recv()
        pl.when(inside(there))(lambda: line_copy(source, p, there).start())
        if p == 0:
            with jax.named_scope("notewait"):
                note_copy(source, mine).wait_recv()
            pl.when(inside(there))(lambda: note_copy(source, there).start())

    def take_line(step, p):
        for side in sides:
            pl.when(inside(mine + side * step))(functools.partial(pass_on, step, side, p))

    def take_pair(d):
        for p in range(2):
            with jax.named_scope("pairwait"):
                pair_copy(d, p).wait_recv()
            relay_copy(d, p, core).start()

    def take_core(d):
        with jax.named_scope("corewait"):
            for p in range(2):
                core_copy(d, p, other).wait_recv()
                relay_copy(d, p, other).wait_recv()

    def compute(d, h):
        block = jnp.concatenate([rows[d, 0, unit(h), :], rows[d, 1, unit(h), :]], axis=0)
        pre = jnp.dot(block, gate_up[...], preferred_element_type=jnp.float32)
        gate_pre = pre[:, :hidden_width]
        hidden = (gate_pre / (1.0 + jnp.exp(-gate_pre)) * pre[:, hidden_width:]).astype(
            jnp.bfloat16
        )
        partial = jnp.dot(hidden, down[...], preferred_element_type=jnp.float32)
        parts[d, both(h), :] = partial.astype(jnp.bfloat16)
        part_copy(d, h).start()

    def cross(d, h):
        with jax.named_scope("partwait"):
            part_copy(d, h).wait_recv()
        crossing[d, unit(h)] = (
            parts[d, side_unit(h, 1), own_cols].astype(jnp.float32)
            + peer_parts[d, side_unit(h, 1)].astype(jnp.float32)
        ).astype(jnp.bfloat16)
        cross_copy(d, h).start()

    def meet(d, h):
        with jax.named_scope("crosswait"):
            cross_copy(d, h).wait_recv()
        return (
            parts[d, side_unit(h, 0), own_cols].astype(jnp.float32)
            + peer_parts[d, side_unit(h, 0)].astype(jnp.float32)
            + crossed[d, unit(h)].astype(jnp.float32)
        ).astype(jnp.bfloat16)

    def send_home(d, h):
        leaving[d, unit(h)] = meet(d, h)
        home_copy(d, h).start()

    last = experts - 1
    for p in range(2):
        fill(mine, p, tok_ref[:, cut(p)])
    take_line(1, 0)
    fill_step(1, 0)
    take_pair(mine)
    take_line(1, 1)
    fill_step(1, 1)

    def fill_both(step):
        for p in range(2):
            fill_step(step, p)

    pl.when(inner)(lambda: fill_both(2))
    with jax.named_scope("wwait"):
        for load in loads:
            load.wait()

    def step_of(d, carry):
        now, past = at_step(d), at_step(d - 1)
        early = (d >= 2) | ((d == 1) & inner)
        early_past = (d >= 3) | ((d == 2) & inner)

        def next_line():
            take_line(d + 1, 1)
            pl.when(at_end)(lambda: fill_step(d + 1, 1))

        pl.when(d >= 1)(lambda: take_pair(now))
        pl.when((d >= 2) & (d < last))(next_line)
        take_core(now)
        compute(now, 0)
        pl.when(early_past)(lambda: send_home(past, 0))
        pl.when(d == 1)(next_line)
        compute(now, 1)
        pl.when(early)(lambda: cross(now, 0))
        pl.when(d + 2 <= last)(lambda: take_line(d + 2, 0))
        pl.when(early_past)(lambda: send_home(past, 1))
        pl.when(early)(lambda: cross(now, 1))
        pl.when((d + 2 <= last) & at_end)(lambda: fill_step(d + 2, 0))
        pl.when((d >= 1) & (d + 2 <= last) & inner)(lambda: fill_both(d + 2))
        return carry

    lax.fori_loop(0, experts, step_of, 0)

    def weights_of(expert, h):
        names = slots(expert, begin[h], size[h])
        mix = jnp.where(names == target_one, route_ref[0:1, :], 0.0) + jnp.where(
            names == target_two, route_ref[1:2, :], 0.0
        )
        high = mix.astype(jnp.bfloat16)
        return high, (mix - high.astype(jnp.float32)).astype(jnp.bfloat16)

    def combine(expert, h):
        dims = (((0,), (0,)), ((), ()))
        high, low = weights_of(expert, h)
        values = home[expert, unit(h)]
        return lax.dot_general(
            high, values, dims, preferred_element_type=jnp.float32
        ) + lax.dot_general(low, values, dims, preferred_element_type=jnp.float32)

    def take_home(expert, h):
        with jax.named_scope("homewait"):
            home_arrival(expert, h).wait_recv()
        total[...] += combine(expert, h)

    def late_cross():
        for h in range(2):
            cross(at_step(1), h)

    def late_home():
        for h in range(2):
            send_home(at_step(1), h)

    pl.when(at_end)(late_cross)
    for h in range(2):
        cross(mine, h)
    for h in range(2):
        send_home(at_step(last), h)
    pl.when(at_end)(late_home)
    home[mine, unit(0)] = meet(mine, 0)
    total[...] = combine(mine, 0)
    for step in range(1, experts):
        take_home(at_step(step), 0)
    home[mine, unit(1)] = meet(mine, 1)
    total[...] += combine(mine, 1)
    for step in range(1, experts):
        take_home(at_step(step), 1)
    routed = total[...]
    sums[...] = jnp.broadcast_to(jnp.sum(routed * routed, axis=1, keepdims=True), (tok_rows, 128))
    sum_copy().start()
    with jax.named_scope("sum1"):
        sum_copy().wait_recv()
    squares_out = sums[...] + peer_sums[...]
    factor_out = lax.rsqrt(squares_out[:, 0:1] / (2 * width) + norm_eps)
    out_ref[...] = (total[...] * factor_out * gain_out_ref[:, own_cols]).astype(jnp.bfloat16)

    square_copy().wait_send()
    sum_copy().wait_send()

    def drain_own(side):
        own_note(side).wait_send()
        for p in range(2):
            own_copy(side, p).wait_send()

    for side in sides:
        pl.when(inside(mine + side))(functools.partial(drain_own, side))

    def drain_far(d):
        there = jnp.where(d < mine, mine + 1, mine - 1)

        def passed():
            note_copy(d, there).wait_send()
            for p in range(2):
                line_copy(d, p, there).wait_send()

        pl.when(inside(there))(passed)
        for h in range(2):
            home_copy(d, h).wait_send()

    def drain(d, carry):
        for i in range(2):
            core_copy(d, i, core).wait_send()
            pair_copy(d, i).wait_send()
            relay_copy(d, i, core).wait_send()
            part_copy(d, i).wait_send()
            cross_copy(d, i).wait_send()
        pl.when(d != mine)(lambda: drain_far(d))
        return carry

    lax.fori_loop(0, experts, drain, 0)


def layer(
    tokens, gain_in, gain_out, expert_ids, route_weight, gate_weight, up_weight, down_weight
):
    tok_rows, width = tokens.shape
    experts = lax.axis_size("ep") // 2
    picks = expert_ids.shape[1]
    cap = tok_rows * picks * 3 // (2 * experts)
    hidden_width = gate_weight.shape[2]
    if picks != 2 or experts < 3 or cap % 16 or cap < 32 or width % 256 or hidden_width % 128:
        return plain(
            tokens, gain_in, gain_out, expert_ids, route_weight, gate_weight, up_weight, down_weight
        )
    vmem = pl.BlockSpec(memory_space=pltpu.VMEM)
    hbm = pl.BlockSpec(memory_space=pl.ANY)
    bf16, f32 = jnp.bfloat16, jnp.float32
    lines = [pltpu.SemaphoreType.DMA((experts * 2,))] * 14
    return pl.pallas_call(
        functools.partial(fused, experts, cap),
        out_shape=jax.ShapeDtypeStruct((tok_rows, width), bf16),
        in_specs=[vmem] * 5 + [hbm] * 3,
        out_specs=vmem,
        scratch_shapes=[
            pltpu.VMEM((experts, tok_rows, width), bf16),
            pltpu.VMEM((experts, 8, tok_rows), f32),
            pltpu.VMEM((experts, 2, cap, 2 * width), bf16),
            pltpu.VMEM((experts, 2 * cap, 2 * width), bf16),
            pltpu.VMEM((experts, 2 * cap, width), bf16),
            pltpu.VMEM((experts, cap, width), bf16),
            pltpu.VMEM((experts, cap, width), bf16),
            pltpu.VMEM((experts, cap, width), bf16),
            pltpu.VMEM((experts, cap, width), bf16),
            pltpu.VMEM((2 * width, 2 * hidden_width), bf16),
            pltpu.VMEM((hidden_width, 2 * width), bf16),
            pltpu.VMEM((8, tok_rows), f32),
            pltpu.VMEM((8, tok_rows), f32),
            pltpu.VMEM((tok_rows, 128), f32),
            pltpu.VMEM((tok_rows, 128), f32),
            pltpu.VMEM((tok_rows, width), f32),
            pltpu.SemaphoreType.DMA((3,)),
            pltpu.SemaphoreType.DMA((2,)),
            pltpu.SemaphoreType.DMA((2,)),
            pltpu.SemaphoreType.DMA((4,)),
            pltpu.SemaphoreType.DMA((2,)),
            pltpu.SemaphoreType.DMA((experts,)),
            pltpu.SemaphoreType.DMA((experts,)),
        ]
        + lines,
        compiler_params=pltpu.CompilerParams(
            collective_id=0, has_side_effects=True, vmem_limit_bytes=60 * 1024 * 1024
        ),
    )(
        tokens,
        gain_in[None, :],
        gain_out[None, :],
        expert_ids.T,
        route_weight.T,
        gate_weight,
        up_weight,
        down_weight,
    )


def solution(mesh):
    in_specs = (
        P(("grp", "ep"), "tp"),
        P(),
        P(),
        P(("grp", "ep"), None),
        P(("grp", "ep"), None),
        P("ep", None, "tp"),
        P("ep", None, "tp"),
        P("ep", "tp", None),
    )
    out_specs = P(("grp", "ep"), "tp")
    return jax.shard_map(layer, mesh=mesh, in_specs=in_specs, out_specs=out_specs, check_vma=False)
```

```python
import functools

import jax
import jax.numpy as jnp
from jax import lax
from jax.experimental import pallas as pl
from jax.experimental.pallas import tpu as pltpu
from jax.sharding import PartitionSpec as P

norm_eps = 1e-06


def plain(
    tokens, gain_in, gain_out, expert_ids, route_weight, gate_weight, up_weight, down_weight
):
    tok_rows, half_width = tokens.shape
    full_width = 2 * half_width
    expert_count = lax.axis_size("ep") // 2
    picks = expert_ids.shape[1]
    capacity = tok_rows * picks * 3 // (2 * expert_count)
    own_cols = lax.axis_index("tp") * half_width
    own_float = tokens.astype(jnp.float32)
    squares = lax.psum(jnp.sum(own_float * own_float, axis=1), "tp")
    factor = lax.rsqrt(squares / full_width + norm_eps)[:, None]
    own_gain = lax.dynamic_slice_in_dim(gain_in, own_cols, half_width)
    normed = (own_float * factor * own_gain).astype(jnp.bfloat16)
    sent_width = normed.shape[1]
    flat_ids = expert_ids.reshape(-1)
    onehot = (flat_ids[:, None] == jnp.arange(expert_count, dtype=jnp.int32)[None, :]).astype(
        jnp.int32
    )
    before = jnp.cumsum(onehot, axis=0) - onehot
    targets = flat_ids * capacity + jnp.sum(before * onehot, axis=1)
    per_token = targets.reshape(tok_rows, picks)
    slot_rows = jnp.arange(expert_count * capacity, dtype=jnp.int32)[:, None]
    placing = jnp.zeros((expert_count * capacity, tok_rows), jnp.bfloat16)
    for which in range(picks):
        placing = placing + (slot_rows == per_token[None, :, which]).astype(jnp.bfloat16)
    packed = jnp.dot(placing, normed, preferred_element_type=jnp.float32).astype(jnp.bfloat16)
    stacked = packed.reshape(expert_count, 1, capacity, sent_width)
    outgoing = jnp.broadcast_to(stacked, (expert_count, 2, capacity, sent_width)).reshape(
        2 * expert_count, capacity, sent_width
    )
    arrived = lax.all_to_all(outgoing, "ep", split_axis=0, concat_axis=0, tiled=True)
    arrived = lax.all_gather(arrived, "tp", axis=2, tiled=True)
    sources = arrived.shape[0]
    gathered = arrived.reshape(sources * capacity, full_width)
    gate_pre = jnp.dot(gathered, gate_weight[0], preferred_element_type=jnp.float32)
    up_pre = jnp.dot(gathered, up_weight[0], preferred_element_type=jnp.float32)
    hidden = (jax.nn.silu(gate_pre) * up_pre).astype(jnp.bfloat16)
    partial_value = jnp.dot(hidden, down_weight[0], preferred_element_type=jnp.float32).astype(
        jnp.bfloat16
    )
    partial_value = partial_value.reshape(sources, capacity, full_width)
    half_sum = lax.psum_scatter(partial_value, "tp", scatter_dimension=2, tiled=True).astype(
        jnp.float32
    )
    returned = lax.all_to_all(
        half_sum.astype(jnp.bfloat16), "ep", split_axis=0, concat_axis=0, tiled=True
    )
    merged = jnp.sum(
        returned.reshape(expert_count, 2, capacity, half_width).astype(jnp.float32), axis=1
    )
    merged = merged.reshape(expert_count * capacity, half_width)
    picked = jnp.take(merged, targets, axis=0).reshape(tok_rows, picks, half_width)
    routed = jnp.sum(picked * route_weight[:, :, None], axis=1)
    squares_out = lax.psum(jnp.sum(routed * routed, axis=1), "tp")
    factor_out = lax.rsqrt(squares_out / full_width + norm_eps)[:, None]
    own_gain_out = lax.dynamic_slice_in_dim(gain_out, own_cols, half_width)
    return (routed * factor_out * own_gain_out).astype(jnp.bfloat16)


MESH = pl.DeviceIdType.MESH


def fused(
    experts,
    cap,
    tok_hbm,
    gain_in_hbm,
    gain_out_hbm,
    ids_hbm,
    route_hbm,
    gate_hbm,
    up_hbm,
    down_hbm,
    out_ref,
    tok_ref,
    gain_in_ref,
    gain_out_ref,
    ids_ref,
    route_ref,
    arrived,
    notes,
    packed,
    rows,
    parts,
    peer_parts,
    crossing,
    crossed,
    leaving,
    home,
    gate_up,
    down,
    squared,
    peer_squared,
    sums,
    peer_sums,
    total,
    w_sem,
    in_sem,
    sent,
    own_sent,
    line_sent,
    note_sent,
    sq_recv,
    note_recv,
    line_recv,
    rows_recv,
    pair_recv,
    part_recv,
    cross_recv,
    home_recv,
):
    tok_rows, width = tok_ref.shape
    hidden_width = down.shape[0]
    place = lax.axis_index("ep")
    core = lax.axis_index("tp")
    half = place % 2
    mine = place // 2
    partner = place + 1 - 2 * half
    other = 1 - core
    own_cols = pl.ds(pl.multiple_of(core * width, 128), width)
    other_cols = pl.ds(pl.multiple_of(other * width, 128), width)

    size = ((cap // 16 + 1) // 2 * 16, cap // 16 // 2 * 16)
    begin = (0, size[0])

    def unit(h):
        return pl.ds(begin[h], size[h])

    def side_unit(h, which):
        return pl.ds(2 * begin[h] + which * size[h], size[h])

    def both(h):
        return pl.ds(2 * begin[h], 2 * size[h])

    piece = width // 2

    def cut(p):
        return pl.ds(p * piece, piece)

    def of_core(which, p):
        return pl.ds(pl.multiple_of(which * width + p * piece, 128), piece)

    def turn(where):
        return 1 - 2 * ((2 * where) // experts)

    last = experts - 1

    def is_end(where):
        return (where == 0) | (where == last)

    def is_inner(where):
        return (where > 0) & (where < last)

    at_end, inner = is_end(mine), is_inner(mine)

    def at_step(step):
        far = jnp.where(step == 2, experts - 1, jnp.where(step > 2, step - 1, step))
        count = jnp.where(inner, far, step)
        return (mine + turn(mine) * count + experts) % experts

    def on_line(there):
        return {"ep": 2 * there + half}

    loads = [
        pltpu.make_async_copy(gate_hbm.at[0], gate_up.at[:, pl.ds(0, hidden_width)], w_sem.at[0]),
        pltpu.make_async_copy(
            up_hbm.at[0], gate_up.at[:, pl.ds(hidden_width, hidden_width)], w_sem.at[0]
        ),
        pltpu.make_async_copy(down_hbm.at[0], down, w_sem.at[1]),
    ]
    barrier = pltpu.get_barrier_semaphore()
    sides = (-1, 1)

    def inside(where):
        return (where >= 0) & (where < experts)

    def greet(side):
        there = on_line(mine + side)
        pl.semaphore_signal(barrier, inc=1, device_id=there, device_id_type=MESH)

    for side in sides:
        pl.when(inside(mine + side))(functools.partial(greet, side))
    pl.semaphore_signal(barrier, inc=1, device_id={"ep": partner}, device_id_type=MESH)
    pl.semaphore_signal(barrier, inc=1, device_id={"tp": other}, device_id_type=MESH)
    inputs = [
        pltpu.make_async_copy(source, target, in_sem.at[i])
        for i, (source, target) in enumerate(
            (
                (tok_hbm, tok_ref),
                (ids_hbm, ids_ref),
                (gain_in_hbm, gain_in_ref),
                (route_hbm, route_ref),
                (gain_out_hbm, gain_out_ref),
            )
        )
    ]
    for load in inputs:
        load.start()

    def remote(source, target, send, recv, device):
        return pltpu.make_async_remote_copy(
            src_ref=source,
            dst_ref=target,
            send_sem=send,
            recv_sem=recv,
            device_id=device,
            device_id_type=MESH,
        )

    def square_copy():
        return remote(squared, peer_squared, sent.at[0], sq_recv.at[0], {"tp": other})

    def sum_copy():
        return remote(sums, peer_sums, sent.at[1], sq_recv.at[1], {"tp": other})

    def own_copy(side, p):
        return remote(
            tok_ref.at[:, cut(p)],
            arrived.at[mine, :, cut(p)],
            own_sent.at[(side + 1) // 2],
            line_recv.at[2 * mine + p],
            on_line(mine + side),
        )

    def own_note(side):
        return remote(
            notes.at[mine],
            notes.at[mine],
            own_sent.at[2 + (side + 1) // 2],
            note_recv.at[mine],
            on_line(mine + side),
        )

    def line_copy(source, p, there):
        view = arrived.at[source, :, cut(p)]
        return remote(
            view, view, line_sent.at[source], line_recv.at[2 * source + p], on_line(there)
        )

    def note_copy(source, there):
        view = notes.at[source]
        return remote(view, view, note_sent.at[source], note_recv.at[source], on_line(there))

    def box_copy(source, p, there):
        return remote(
            packed.at[source, :, cut(p)],
            rows.at[source, 0, :, of_core(core, p)],
            sent.at[3],
            line_recv.at[2 * source + p],
            on_line(there),
        )

    def core_copy(d, p):
        view = rows.at[d, 0, :, of_core(core, p)]
        return remote(view, view, sent.at[4], rows_recv.at[d], {"tp": other})

    def pair_copy(d, p):
        return remote(
            rows.at[d, 0, :, of_core(core, p)],
            rows.at[d, 1, :, of_core(core, p)],
            sent.at[5],
            pair_recv.at[2 * d + p],
            {"ep": partner},
        )

    def relay_copy(d, p):
        view = rows.at[d, 1, :, of_core(core, p)]
        return remote(view, view, sent.at[4], rows_recv.at[d], {"tp": other})

    def other_half(d):
        view = rows.at[d, :, :, other_cols]
        return remote(view, view, sent.at[4], rows_recv.at[d], {"tp": other})

    def part_copy(d, h):
        return remote(
            parts.at[d, both(h), other_cols],
            peer_parts.at[d, both(h)],
            sent.at[6],
            part_recv.at[2 * d + h],
            {"tp": other},
        )

    def cross_copy(d, h):
        return remote(
            crossing.at[d, unit(h)],
            crossed.at[d, unit(h)],
            sent.at[7],
            cross_recv.at[2 * d + h],
            {"ep": partner},
        )

    def home_copy(d, h):
        return remote(
            leaving.at[d, unit(h)],
            home.at[mine, unit(h)],
            sent.at[8],
            home_recv.at[2 * mine + h],
            on_line(d),
        )

    def home_arrival(expert, h):
        view = home.at[expert, unit(h)]
        return remote(view, view, sent.at[8], home_recv.at[2 * expert + h], on_line(expert))

    inputs[0].wait()
    with jax.named_scope("barrier"):
        pl.semaphore_wait(
            barrier, 2 + (mine > 0).astype(jnp.int32) + (mine < experts - 1).astype(jnp.int32)
        )

    def own_out(side, p):
        own_copy(side, p).start()

    def own_note_out(side):
        own_note(side).start()

    for side in sides:
        pl.when(is_inner(mine + side))(functools.partial(own_out, side, 0))
    own_float = tok_ref[...].astype(jnp.float32)
    squares = jnp.broadcast_to(
        jnp.sum(own_float * own_float, axis=1, keepdims=True), (tok_rows, 128)
    )
    squared[...] = squares.T[0:8, :]
    square_copy().start()
    for load in loads:
        load.start()
    for load in inputs[1:]:
        load.wait()
    lead = max(8, experts)
    names = lax.broadcasted_iota(jnp.int32, (lead, tok_rows), 0)
    first = names == ids_ref[0:1, :]
    second = names == ids_ref[1:2, :]
    either = (first.astype(jnp.float32) + second.astype(jnp.float32)).astype(jnp.bfloat16)
    earlier = (
        lax.broadcasted_iota(jnp.int32, (tok_rows, tok_rows), 0)
        < lax.broadcasted_iota(jnp.int32, (tok_rows, tok_rows), 1)
    ).astype(jnp.float32).astype(jnp.bfloat16)
    before = jnp.dot(either, earlier, preferred_element_type=jnp.float32)
    slot_one = jnp.sum(jnp.where(first, before, 0.0), axis=0, keepdims=True).astype(jnp.int32)
    slot_two = jnp.sum(jnp.where(second, before, 0.0), axis=0, keepdims=True).astype(jnp.int32)
    target_one = (ids_ref[0:1, :] * cap + slot_one).astype(jnp.float32)
    target_two = (ids_ref[1:2, :] * cap + slot_two).astype(jnp.float32)

    def slots(expert, first_row, count):
        names = lax.broadcasted_iota(jnp.int32, (count, tok_rows), 0) + expert * cap + first_row
        return names.astype(jnp.float32)

    with jax.named_scope("sum0"):
        square_copy().wait_recv()
    factor = lax.rsqrt((squared[...] + peer_squared[...]) / (2 * width) + norm_eps)
    row = lax.broadcasted_iota(jnp.int32, (8, tok_rows), 0)
    notes[mine] = jnp.where(row == 0, target_one, jnp.where(row == 1, target_two, factor))
    for side in sides:
        pl.when(is_inner(mine + side))(functools.partial(own_note_out, side))
    for side in sides:
        pl.when(is_inner(mine + side))(functools.partial(own_out, side, 1))

    def pack(source, p, tokens, expert):
        one, two, scale = (notes[source, i : i + 1, :] for i in range(3))
        names = slots(expert, 0, cap)
        placing = jnp.where((names == one) | (names == two), scale, 0.0)
        high = placing.astype(jnp.bfloat16)
        low = (placing - high.astype(jnp.float32)).astype(jnp.bfloat16)
        values = jnp.dot(high, tokens, preferred_element_type=jnp.float32) + jnp.dot(
            low, tokens, preferred_element_type=jnp.float32
        )
        return (values * gain_in_ref[:, of_core(core, p)]).astype(jnp.bfloat16)

    def launch(source, p):
        pair_copy(source, p).start()
        core_copy(source, p).start()

    def fill_step(step, p):
        source = at_step(step)

        def fill():
            rows[source, 0, :, of_core(core, p)] = pack(
                source, p, arrived[source, :, cut(p)], mine
            )

        pl.when(inner)(fill)
        launch(source, p)

    def box_out(source, p, tokens, there):
        packed[source, :, cut(p)] = pack(source, p, tokens, there)
        box_copy(source, p, there).start()

    def pass_on(step, side, p):
        source, there = mine + side * step, mine - side

        def take_box():
            with jax.named_scope("boxwait"):
                box_copy(source, p, mine).wait_recv()

        def take_tokens():
            with jax.named_scope("linewait"):
                line_copy(source, p, mine).wait_recv()
            pl.when(is_inner(there))(lambda: line_copy(source, p, there).start())
            if p == 0:
                with jax.named_scope("notewait"):
                    note_copy(source, mine).wait_recv()
                pl.when(is_inner(there))(lambda: note_copy(source, there).start())
            pl.when(is_end(there))(
                lambda: box_out(source, p, arrived[source, :, cut(p)], there)
            )

        pl.when(at_end)(take_box)
        pl.when(inner)(take_tokens)

    def take_line(step, p):
        for side in sides:
            pl.when(inside(mine + side * step))(functools.partial(pass_on, step, side, p))

    def take_pair(d):
        for p in range(2):
            with jax.named_scope("pairwait"):
                pair_copy(d, p).wait_recv()
            relay_copy(d, p).start()

    def take_core(d):
        with jax.named_scope("corewait"):
            other_half(d).wait_recv()

    def compute(d, h):
        block = jnp.concatenate([rows[d, 0, unit(h), :], rows[d, 1, unit(h), :]], axis=0)
        pre = jnp.dot(block, gate_up[...], preferred_element_type=jnp.float32)
        gate_pre = pre[:, :hidden_width]
        hidden = (gate_pre / (1.0 + jnp.exp(-gate_pre)) * pre[:, hidden_width:]).astype(
            jnp.bfloat16
        )
        partial = jnp.dot(hidden, down[...], preferred_element_type=jnp.float32)
        parts[d, both(h), :] = partial.astype(jnp.bfloat16)
        part_copy(d, h).start()

    def cross(d, h):
        with jax.named_scope("partwait"):
            part_copy(d, h).wait_recv()
        crossing[d, unit(h)] = (
            parts[d, side_unit(h, 1), own_cols].astype(jnp.float32)
            + peer_parts[d, side_unit(h, 1)].astype(jnp.float32)
        ).astype(jnp.bfloat16)
        cross_copy(d, h).start()

    def meet(d, h):
        with jax.named_scope("crosswait"):
            cross_copy(d, h).wait_recv()
        return (
            parts[d, side_unit(h, 0), own_cols].astype(jnp.float32)
            + peer_parts[d, side_unit(h, 0)].astype(jnp.float32)
            + crossed[d, unit(h)].astype(jnp.float32)
        ).astype(jnp.bfloat16)

    def send_home(d, h):
        leaving[d, unit(h)] = meet(d, h)
        home_copy(d, h).start()

    last = experts - 1
    for p in range(2):
        rows[mine, 0, :, of_core(core, p)] = pack(mine, p, tok_ref[:, cut(p)], mine)
        launch(mine, p)
        for side in sides:
            there = mine + side
            pl.when(inner & is_end(there))(
                functools.partial(lambda p, there: box_out(mine, p, tok_ref[:, cut(p)], there), p, there)
            )
    take_line(1, 0)
    fill_step(1, 0)
    take_pair(mine)
    take_line(1, 1)
    fill_step(1, 1)

    def fill_both(step):
        for p in range(2):
            fill_step(step, p)

    pl.when(inner)(lambda: fill_both(2))
    with jax.named_scope("wwait"):
        pltpu.make_async_copy(gate_up, gate_up, w_sem.at[0]).wait()
        loads[2].wait()

    def step_of(d, carry):
        now, past = at_step(d), at_step(d - 1)
        early = (d >= 2) | ((d == 1) & inner)

        def next_line():
            take_line(d + 1, 1)
            pl.when(at_end)(lambda: fill_step(d + 1, 1))
            pl.when(inner & (d + 2 <= last))(lambda: fill_step(d + 2, 1))

        pl.when(d >= 1)(lambda: take_pair(now))
        pl.when((d >= 1) & (d < last) & (at_end | (d >= 2)))(next_line)
        take_core(now)
        compute(now, 0)
        pl.when((d >= 3) & inner)(lambda: send_home(at_step(d - 2), 1))
        pl.when((d >= 3) & at_end)(lambda: send_home(past, 0))
        pl.when((d == 1) & inner)(next_line)
        compute(now, 1)
        pl.when(early)(lambda: cross(now, 0))
        pl.when((d >= 2) & inner)(lambda: send_home(past, 0))
        pl.when((d >= 3) & at_end)(lambda: send_home(past, 1))
        pl.when(d + 2 <= last)(lambda: take_line(d + 2, 0))
        pl.when(early)(lambda: cross(now, 1))
        pl.when((d + 2 <= last) & at_end)(lambda: fill_step(d + 2, 0))
        pl.when((d + 3 <= last) & inner)(lambda: fill_step(d + 3, 0))
        return carry

    lax.fori_loop(0, experts, step_of, 0)

    def weights_of(expert, h):
        names = slots(expert, begin[h], size[h])
        mix = jnp.where(names == target_one, route_ref[0:1, :], 0.0) + jnp.where(
            names == target_two, route_ref[1:2, :], 0.0
        )
        high = mix.astype(jnp.bfloat16)
        return high, (mix - high.astype(jnp.float32)).astype(jnp.bfloat16)

    def combine(expert, h):
        dims = (((0,), (0,)), ((), ()))
        high, low = weights_of(expert, h)
        values = home[expert, unit(h)]
        return lax.dot_general(
            high, values, dims, preferred_element_type=jnp.float32
        ) + lax.dot_general(low, values, dims, preferred_element_type=jnp.float32)

    def take_home(expert, h):
        with jax.named_scope("homewait"):
            home_arrival(expert, h).wait_recv()
        total[...] += combine(expert, h)

    def end_rest():
        for h in range(2):
            cross(at_step(1), h)
        for h in range(2):
            cross(mine, h)
        for step in (last, 1):
            for h in range(2):
                send_home(at_step(step), h)

    def inner_rest():
        for h in range(2):
            cross(mine, h)
        send_home(at_step(last - 1), 1)
        for h in range(2):
            send_home(at_step(last), h)

    pl.when(at_end)(end_rest)
    pl.when(inner)(inner_rest)
    home[mine, unit(0)] = meet(mine, 0)
    total[...] = combine(mine, 0)
    waited = [step for step in range(1, experts) if step != 2] + [2] * (experts > 2)
    for step in waited:
        take_home(at_step(step), 0)
    home[mine, unit(1)] = meet(mine, 1)
    total[...] += combine(mine, 1)
    for step in waited:
        take_home(at_step(step), 1)
    routed = total[...]
    sums[...] = jnp.broadcast_to(jnp.sum(routed * routed, axis=1, keepdims=True), (tok_rows, 128))
    sum_copy().start()
    with jax.named_scope("sum1"):
        sum_copy().wait_recv()
    squares_out = sums[...] + peer_sums[...]
    factor_out = lax.rsqrt(squares_out[:, 0:1] / (2 * width) + norm_eps)
    out_ref[...] = (total[...] * factor_out * gain_out_ref[:, own_cols]).astype(jnp.bfloat16)

    def sent_all(view, sem):
        pltpu.make_async_remote_copy(
            src_ref=view,
            dst_ref=view,
            send_sem=sem,
            recv_sem=sq_recv.at[0],
            device_id={"tp": other},
            device_id_type=MESH,
        ).wait_send()

    others = pl.ds(0, last)
    for side in sides:

        def own_done(side=side):
            sent_all(tok_ref, own_sent.at[(side + 1) // 2])
            own_note(side).wait_send()

        pl.when(is_inner(mine + side))(own_done)
        pl.when(inner & is_end(mine + side))(lambda: sent_all(packed.at[others], sent.at[3]))

    def forwarded(source, carry):
        def done():
            sent_all(notes.at[source], note_sent.at[source])
            sent_all(arrived.at[source], line_sent.at[source])

        up = (source < mine) & is_inner(mine + 1)
        pl.when(inner & (up | ((source > mine) & is_inner(mine - 1))))(done)
        return carry

    lax.fori_loop(0, experts, forwarded, 0)
    sent_all(rows.at[:, :, :, pl.ds(0, width)], sent.at[4])
    sent_all(rows.at[:, 0, :, pl.ds(0, width)], sent.at[5])
    sent_all(parts.at[:, :, pl.ds(0, width)], sent.at[6])
    sent_all(crossing, sent.at[7])
    sent_all(leaving.at[others], sent.at[8])
    square_copy().wait_send()
    sum_copy().wait_send()


def layer(
    tokens, gain_in, gain_out, expert_ids, route_weight, gate_weight, up_weight, down_weight
):
    tok_rows, width = tokens.shape
    experts = lax.axis_size("ep") // 2
    picks = expert_ids.shape[1]
    cap = tok_rows * picks * 3 // (2 * experts)
    hidden_width = gate_weight.shape[2]
    if picks != 2 or experts < 4 or cap % 16 or cap < 32 or width % 256 or hidden_width % 128:
        return plain(
            tokens, gain_in, gain_out, expert_ids, route_weight, gate_weight, up_weight, down_weight
        )
    vmem = pl.BlockSpec(memory_space=pltpu.VMEM)
    hbm = pl.BlockSpec(memory_space=pl.ANY)
    bf16, f32 = jnp.bfloat16, jnp.float32
    dma = pltpu.SemaphoreType.DMA
    return pl.pallas_call(
        functools.partial(fused, experts, cap),
        out_shape=pltpu.VMEM((tok_rows, width), bf16),
        in_specs=[hbm] * 8,
        out_specs=vmem,
        scratch_shapes=[
            pltpu.VMEM((tok_rows, width), bf16),
            pltpu.VMEM((1, 2 * width), f32),
            pltpu.VMEM((1, 2 * width), f32),
            pltpu.VMEM((picks, tok_rows), jnp.int32),
            pltpu.VMEM((picks, tok_rows), f32),
            pltpu.VMEM((experts, tok_rows, width), bf16),
            pltpu.VMEM((experts, 8, tok_rows), f32),
            pltpu.VMEM((experts, cap, width), bf16),
            pltpu.VMEM((experts, 2, cap, 2 * width), bf16),
            pltpu.VMEM((experts, 2 * cap, 2 * width), bf16),
            pltpu.VMEM((experts, 2 * cap, width), bf16),
            pltpu.VMEM((experts, cap, width), bf16),
            pltpu.VMEM((experts, cap, width), bf16),
            pltpu.VMEM((experts, cap, width), bf16),
            pltpu.VMEM((experts, cap, width), bf16),
            pltpu.VMEM((2 * width, 2 * hidden_width), bf16),
            pltpu.VMEM((hidden_width, 2 * width), bf16),
            pltpu.VMEM((8, tok_rows), f32),
            pltpu.VMEM((8, tok_rows), f32),
            pltpu.VMEM((tok_rows, 128), f32),
            pltpu.VMEM((tok_rows, 128), f32),
            pltpu.VMEM((tok_rows, width), f32),
            dma((2,)),
            dma((5,)),
            dma((9,)),
            dma((4,)),
            dma((experts,)),
            dma((experts,)),
            dma((2,)),
            dma((experts,)),
            dma((2 * experts,)),
            dma((experts,)),
            dma((2 * experts,)),
            dma((2 * experts,)),
            dma((2 * experts,)),
            dma((2 * experts,)),
        ],
        compiler_params=pltpu.CompilerParams(
            collective_id=0, has_side_effects=True, vmem_limit_bytes=60 * 1024 * 1024
        ),
    )(
        tokens,
        gain_in[None, :],
        gain_out[None, :],
        expert_ids.T,
        route_weight.T,
        gate_weight,
        up_weight,
        down_weight,
    )


def solution(mesh):
    in_specs = (
        P(("grp", "ep"), "tp"),
        P(),
        P(),
        P(("grp", "ep"), None),
        P(("grp", "ep"), None),
        P("ep", None, "tp"),
        P("ep", None, "tp"),
        P("ep", "tp", None),
    )
    out_specs = P(("grp", "ep"), "tp")
    return jax.shard_map(layer, mesh=mesh, in_specs=in_specs, out_specs=out_specs, check_vma=False)
```

```python
import functools

import jax
import jax.numpy as jnp
from jax import lax
from jax.experimental import pallas as pl
from jax.experimental.pallas import tpu as pltpu
from jax.sharding import PartitionSpec as P

norm_eps = 1e-06


def plain(
    tokens, gain_in, gain_out, expert_ids, route_weight, gate_weight, up_weight, down_weight
):
    tok_rows, half_width = tokens.shape
    full_width = 2 * half_width
    expert_count = lax.axis_size("ep") // 2
    picks = expert_ids.shape[1]
    capacity = tok_rows * picks * 3 // (2 * expert_count)
    own_cols = lax.axis_index("tp") * half_width
    own_float = tokens.astype(jnp.float32)
    squares = lax.psum(jnp.sum(own_float * own_float, axis=1), "tp")
    factor = lax.rsqrt(squares / full_width + norm_eps)[:, None]
    own_gain = lax.dynamic_slice_in_dim(gain_in, own_cols, half_width)
    normed = (own_float * factor * own_gain).astype(jnp.bfloat16)
    sent_width = normed.shape[1]
    flat_ids = expert_ids.reshape(-1)
    onehot = (flat_ids[:, None] == jnp.arange(expert_count, dtype=jnp.int32)[None, :]).astype(
        jnp.int32
    )
    before = jnp.cumsum(onehot, axis=0) - onehot
    targets = flat_ids * capacity + jnp.sum(before * onehot, axis=1)
    per_token = targets.reshape(tok_rows, picks)
    slot_rows = jnp.arange(expert_count * capacity, dtype=jnp.int32)[:, None]
    placing = jnp.zeros((expert_count * capacity, tok_rows), jnp.bfloat16)
    for which in range(picks):
        placing = placing + (slot_rows == per_token[None, :, which]).astype(jnp.bfloat16)
    packed = jnp.dot(placing, normed, preferred_element_type=jnp.float32).astype(jnp.bfloat16)
    stacked = packed.reshape(expert_count, 1, capacity, sent_width)
    outgoing = jnp.broadcast_to(stacked, (expert_count, 2, capacity, sent_width)).reshape(
        2 * expert_count, capacity, sent_width
    )
    arrived = lax.all_to_all(outgoing, "ep", split_axis=0, concat_axis=0, tiled=True)
    arrived = lax.all_gather(arrived, "tp", axis=2, tiled=True)
    sources = arrived.shape[0]
    gathered = arrived.reshape(sources * capacity, full_width)
    gate_pre = jnp.dot(gathered, gate_weight[0], preferred_element_type=jnp.float32)
    up_pre = jnp.dot(gathered, up_weight[0], preferred_element_type=jnp.float32)
    hidden = (jax.nn.silu(gate_pre) * up_pre).astype(jnp.bfloat16)
    partial_value = jnp.dot(hidden, down_weight[0], preferred_element_type=jnp.float32).astype(
        jnp.bfloat16
    )
    partial_value = partial_value.reshape(sources, capacity, full_width)
    half_sum = lax.psum_scatter(partial_value, "tp", scatter_dimension=2, tiled=True).astype(
        jnp.float32
    )
    returned = lax.all_to_all(
        half_sum.astype(jnp.bfloat16), "ep", split_axis=0, concat_axis=0, tiled=True
    )
    merged = jnp.sum(
        returned.reshape(expert_count, 2, capacity, half_width).astype(jnp.float32), axis=1
    )
    merged = merged.reshape(expert_count * capacity, half_width)
    picked = jnp.take(merged, targets, axis=0).reshape(tok_rows, picks, half_width)
    routed = jnp.sum(picked * route_weight[:, :, None], axis=1)
    squares_out = lax.psum(jnp.sum(routed * routed, axis=1), "tp")
    factor_out = lax.rsqrt(squares_out / full_width + norm_eps)[:, None]
    own_gain_out = lax.dynamic_slice_in_dim(gain_out, own_cols, half_width)
    return (routed * factor_out * own_gain_out).astype(jnp.bfloat16)


MESH = pl.DeviceIdType.MESH


def fused(
    experts,
    cap,
    tok_hbm,
    gain_in_hbm,
    gain_out_hbm,
    ids_hbm,
    route_hbm,
    gate_hbm,
    up_hbm,
    down_hbm,
    out_ref,
    tok_ref,
    gain_in_ref,
    gain_out_ref,
    ids_ref,
    route_ref,
    arrived,
    notes,
    packed,
    rows,
    parts,
    peer_parts,
    crossing,
    crossed,
    leaving,
    home,
    gate_up,
    down,
    squared,
    peer_squared,
    sums,
    peer_sums,
    total,
    w_sem,
    in_sem,
    sent,
    own_sent,
    line_sent,
    note_sent,
    sq_recv,
    note_recv,
    line_recv,
    rows_recv,
    pair_recv,
    part_recv,
    cross_recv,
    home_recv,
):
    tok_rows, width = tok_ref.shape
    hidden_width = down.shape[0]
    place = lax.axis_index("ep")
    core = lax.axis_index("tp")
    half = place % 2
    mine = place // 2
    partner = place + 1 - 2 * half
    other = 1 - core
    own_cols = pl.ds(pl.multiple_of(core * width, 128), width)
    other_cols = pl.ds(pl.multiple_of(other * width, 128), width)

    size = ((cap // 16 + 1) // 2 * 16, cap // 16 // 2 * 16)
    begin = (0, size[0])

    def unit(h):
        return pl.ds(begin[h], size[h])

    def side_unit(h, which):
        return pl.ds(2 * begin[h] + which * size[h], size[h])

    def both(h):
        return pl.ds(2 * begin[h], 2 * size[h])

    piece = width // 2

    def cut(p):
        return pl.ds(p * piece, piece)

    def of_core(which, p):
        return pl.ds(pl.multiple_of(which * width + p * piece, 128), piece)

    def turn(where):
        return 1 - 2 * ((2 * where) // experts)

    last = experts - 1

    def is_end(where):
        return (where == 0) | (where == last)

    def is_inner(where):
        return (where > 0) & (where < last)

    at_end, inner = is_end(mine), is_inner(mine)

    def at_step(step):
        far = jnp.where(step == 2, experts - 1, jnp.where(step > 2, step - 1, step))
        count = jnp.where(inner, far, step)
        return (mine + turn(mine) * count + experts) % experts

    def on_line(there):
        return {"ep": 2 * there + half}

    loads = [
        pltpu.make_async_copy(gate_hbm.at[0], gate_up.at[:, pl.ds(0, hidden_width)], w_sem.at[0]),
        pltpu.make_async_copy(
            up_hbm.at[0], gate_up.at[:, pl.ds(hidden_width, hidden_width)], w_sem.at[0]
        ),
        pltpu.make_async_copy(down_hbm.at[0], down, w_sem.at[1]),
    ]
    barrier = pltpu.get_barrier_semaphore()
    sides = (-1, 1)

    def inside(where):
        return (where >= 0) & (where < experts)

    def greet(side):
        there = on_line(mine + side)
        pl.semaphore_signal(barrier, inc=1, device_id=there, device_id_type=MESH)

    for side in sides:
        pl.when(inside(mine + side))(functools.partial(greet, side))
    pl.semaphore_signal(barrier, inc=1, device_id={"ep": partner}, device_id_type=MESH)
    pl.semaphore_signal(barrier, inc=1, device_id={"tp": other}, device_id_type=MESH)
    inputs = [
        pltpu.make_async_copy(source, target, in_sem.at[i])
        for i, (source, target) in enumerate(
            (
                (tok_hbm, tok_ref),
                (ids_hbm, ids_ref),
                (gain_in_hbm, gain_in_ref),
                (route_hbm, route_ref),
                (gain_out_hbm, gain_out_ref),
            )
        )
    ]
    for load in inputs:
        load.start()

    def remote(source, target, send, recv, device):
        return pltpu.make_async_remote_copy(
            src_ref=source,
            dst_ref=target,
            send_sem=send,
            recv_sem=recv,
            device_id=device,
            device_id_type=MESH,
        )

    def square_copy():
        return remote(squared, peer_squared, sent.at[0], sq_recv.at[0], {"tp": other})

    def sum_copy():
        return remote(sums, peer_sums, sent.at[1], sq_recv.at[1], {"tp": other})

    def own_copy(side, p):
        return remote(
            tok_ref.at[:, cut(p)],
            arrived.at[mine, :, cut(p)],
            own_sent.at[(side + 1) // 2],
            line_recv.at[2 * mine + p],
            on_line(mine + side),
        )

    def own_note(side):
        return remote(
            notes.at[mine],
            notes.at[mine],
            own_sent.at[2 + (side + 1) // 2],
            note_recv.at[mine],
            on_line(mine + side),
        )

    def line_copy(source, p, there):
        view = arrived.at[source, :, cut(p)]
        return remote(
            view, view, line_sent.at[source], line_recv.at[2 * source + p], on_line(there)
        )

    def note_copy(source, there):
        view = notes.at[source]
        return remote(view, view, note_sent.at[source], note_recv.at[source], on_line(there))

    def box_copy(source, p, there):
        return remote(
            packed.at[source, :, cut(p)],
            rows.at[source, 0, :, of_core(core, p)],
            sent.at[3],
            line_recv.at[2 * source + p],
            on_line(there),
        )

    def core_copy(d, p):
        view = rows.at[d, 0, :, of_core(core, p)]
        return remote(view, view, sent.at[4], rows_recv.at[d], {"tp": other})

    def pair_copy(d, p):
        return remote(
            rows.at[d, 0, :, of_core(core, p)],
            rows.at[d, 1, :, of_core(core, p)],
            sent.at[5],
            pair_recv.at[2 * d + p],
            {"ep": partner},
        )

    def relay_copy(d, p):
        view = rows.at[d, 1, :, of_core(core, p)]
        return remote(view, view, sent.at[4], rows_recv.at[d], {"tp": other})

    def other_half(d):
        view = rows.at[d, :, :, other_cols]
        return remote(view, view, sent.at[4], rows_recv.at[d], {"tp": other})

    def part_copy(d, h):
        return remote(
            parts.at[d, both(h), other_cols],
            peer_parts.at[d, both(h)],
            sent.at[6],
            part_recv.at[2 * d + h],
            {"tp": other},
        )

    def cross_copy(d, h):
        return remote(
            crossing.at[d, unit(h)],
            crossed.at[d, unit(h)],
            sent.at[7],
            cross_recv.at[2 * d + h],
            {"ep": partner},
        )

    def home_copy(d, h):
        return remote(
            leaving.at[d, unit(h)],
            home.at[mine, unit(h)],
            sent.at[8],
            home_recv.at[2 * mine + h],
            on_line(d),
        )

    def home_arrival(expert, h):
        view = home.at[expert, unit(h)]
        return remote(view, view, sent.at[8], home_recv.at[2 * expert + h], on_line(expert))

    inputs[0].wait()
    with jax.named_scope("barrier"):
        pl.semaphore_wait(
            barrier, 2 + (mine > 0).astype(jnp.int32) + (mine < experts - 1).astype(jnp.int32)
        )

    def own_out(side, p):
        own_copy(side, p).start()

    def own_note_out(side):
        own_note(side).start()

    for side in sides:
        pl.when(is_inner(mine + side))(functools.partial(own_out, side, 0))
    own_float = tok_ref[...].astype(jnp.float32)
    squares = jnp.broadcast_to(
        jnp.sum(own_float * own_float, axis=1, keepdims=True), (tok_rows, 128)
    )
    squared[...] = squares.T[0:8, :]
    square_copy().start()
    for load in loads:
        load.start()
    for load in inputs[1:]:
        load.wait()
    lead = max(8, experts)
    names = lax.broadcasted_iota(jnp.int32, (lead, tok_rows), 0)
    first = names == ids_ref[0:1, :]
    second = names == ids_ref[1:2, :]
    either = (first.astype(jnp.float32) + second.astype(jnp.float32)).astype(jnp.bfloat16)
    earlier = (
        lax.broadcasted_iota(jnp.int32, (tok_rows, tok_rows), 0)
        < lax.broadcasted_iota(jnp.int32, (tok_rows, tok_rows), 1)
    ).astype(jnp.float32).astype(jnp.bfloat16)
    before = jnp.dot(either, earlier, preferred_element_type=jnp.float32)
    slot_one = jnp.sum(jnp.where(first, before, 0.0), axis=0, keepdims=True).astype(jnp.int32)
    slot_two = jnp.sum(jnp.where(second, before, 0.0), axis=0, keepdims=True).astype(jnp.int32)
    target_one = (ids_ref[0:1, :] * cap + slot_one).astype(jnp.float32)
    target_two = (ids_ref[1:2, :] * cap + slot_two).astype(jnp.float32)

    def slots(expert, first_row, count):
        names = lax.broadcasted_iota(jnp.int32, (count, tok_rows), 0) + expert * cap + first_row
        return names.astype(jnp.float32)

    with jax.named_scope("sum0"):
        square_copy().wait_recv()
    factor = lax.rsqrt((squared[...] + peer_squared[...]) / (2 * width) + norm_eps)
    row = lax.broadcasted_iota(jnp.int32, (8, tok_rows), 0)
    notes[mine] = jnp.where(row == 0, target_one, jnp.where(row == 1, target_two, factor))
    for side in sides:
        pl.when(is_inner(mine + side))(functools.partial(own_note_out, side))
    for side in sides:
        pl.when(is_inner(mine + side))(functools.partial(own_out, side, 1))

    def pack(source, p, tokens, expert):
        one, two, scale = (notes[source, i : i + 1, :] for i in range(3))
        names = slots(expert, 0, cap)
        placing = jnp.where((names == one) | (names == two), scale, 0.0)
        high = placing.astype(jnp.bfloat16)
        low = (placing - high.astype(jnp.float32)).astype(jnp.bfloat16)
        values = jnp.dot(high, tokens, preferred_element_type=jnp.float32) + jnp.dot(
            low, tokens, preferred_element_type=jnp.float32
        )
        return (values * gain_in_ref[:, of_core(core, p)]).astype(jnp.bfloat16)

    def launch(source, p):
        pair_copy(source, p).start()
        core_copy(source, p).start()

    def fill_step(step, p):
        source = at_step(step)

        def fill():
            rows[source, 0, :, of_core(core, p)] = pack(
                source, p, arrived[source, :, cut(p)], mine
            )

        pl.when(inner)(fill)
        launch(source, p)

    def box_out(source, p, tokens, there):
        packed[source, :, cut(p)] = pack(source, p, tokens, there)
        box_copy(source, p, there).start()

    def pass_on(step, side, p):
        source, there = mine + side * step, mine - side

        def take_box():
            with jax.named_scope("boxwait"):
                box_copy(source, p, mine).wait_recv()

        def take_tokens():
            with jax.named_scope("linewait"):
                line_copy(source, p, mine).wait_recv()
            pl.when(is_inner(there))(lambda: line_copy(source, p, there).start())
            if p == 0:
                with jax.named_scope("notewait"):
                    note_copy(source, mine).wait_recv()
                pl.when(is_inner(there))(lambda: note_copy(source, there).start())
            pl.when(is_end(there))(
                lambda: box_out(source, p, arrived[source, :, cut(p)], there)
            )

        pl.when(at_end)(take_box)
        pl.when(inner)(take_tokens)

    def take_line(step, p):
        for side in sides:
            pl.when(inside(mine + side * step))(functools.partial(pass_on, step, side, p))

    def take_pair(d):
        for p in range(2):
            with jax.named_scope("pairwait"):
                pair_copy(d, p).wait_recv()
            relay_copy(d, p).start()

    def take_core(d):
        with jax.named_scope("corewait"):
            other_half(d).wait_recv()

    def compute(d, h):
        block = jnp.concatenate([rows[d, 0, unit(h), :], rows[d, 1, unit(h), :]], axis=0)
        pre = jnp.dot(block, gate_up[...], preferred_element_type=jnp.float32)
        gate_pre = pre[:, :hidden_width]
        hidden = (gate_pre / (1.0 + jnp.exp(-gate_pre)) * pre[:, hidden_width:]).astype(
            jnp.bfloat16
        )
        partial = jnp.dot(hidden, down[...], preferred_element_type=jnp.float32)
        parts[d, both(h), :] = partial.astype(jnp.bfloat16)
        part_copy(d, h).start()

    def cross(d, h):
        with jax.named_scope("partwait"):
            part_copy(d, h).wait_recv()
        crossing[d, unit(h)] = (
            parts[d, side_unit(h, 1), own_cols].astype(jnp.float32)
            + peer_parts[d, side_unit(h, 1)].astype(jnp.float32)
        ).astype(jnp.bfloat16)
        cross_copy(d, h).start()

    def meet(d, h):
        with jax.named_scope("crosswait"):
            cross_copy(d, h).wait_recv()
        return (
            parts[d, side_unit(h, 0), own_cols].astype(jnp.float32)
            + peer_parts[d, side_unit(h, 0)].astype(jnp.float32)
            + crossed[d, unit(h)].astype(jnp.float32)
        ).astype(jnp.bfloat16)

    def send_home(d, h):
        leaving[d, unit(h)] = meet(d, h)
        home_copy(d, h).start()

    last = experts - 1
    for p in range(2):
        rows[mine, 0, :, of_core(core, p)] = pack(mine, p, tok_ref[:, cut(p)], mine)
        launch(mine, p)
        for side in sides:
            there = mine + side
            pl.when(inner & is_end(there))(
                functools.partial(lambda p, there: box_out(mine, p, tok_ref[:, cut(p)], there), p, there)
            )
    take_line(1, 0)
    fill_step(1, 0)
    take_pair(mine)
    take_line(1, 1)
    fill_step(1, 1)

    def fill_both(step):
        for p in range(2):
            fill_step(step, p)

    pl.when(inner)(lambda: fill_both(2))
    with jax.named_scope("wwait"):
        pltpu.make_async_copy(gate_up, gate_up, w_sem.at[0]).wait()
        loads[2].wait()

    def step_of(d, carry):
        now, past = at_step(d), at_step(d - 1)
        early = (d >= 2) | ((d == 1) & inner)

        def next_line():
            take_line(d + 1, 1)
            pl.when(at_end)(lambda: fill_step(d + 1, 1))
            pl.when(inner & (d + 2 <= last))(lambda: fill_step(d + 2, 1))

        def line_after():
            take_line(d + 2, 0)
            pl.when(at_end)(lambda: fill_step(d + 2, 0))
            pl.when(inner & (d + 3 <= last))(lambda: fill_step(d + 3, 0))

        pl.when(d >= 1)(lambda: take_pair(now))
        pl.when((d >= 1) & (d < last) & (at_end | (d >= 2)))(next_line)
        take_core(now)
        compute(now, 0)
        pl.when((d >= 3) & inner)(lambda: send_home(at_step(d - 2), 1))
        pl.when((d >= 3) & at_end)(lambda: send_home(past, 0))
        pl.when((d == last) & at_end)(lambda: cross(now, 0))
        pl.when((d == 1) & inner)(next_line)
        compute(now, 1)
        pl.when(early & ((d < last) | inner))(lambda: cross(now, 0))
        pl.when((d >= 2) & inner)(lambda: send_home(past, 0))
        pl.when((d >= 3) & at_end)(lambda: send_home(past, 1))
        pl.when(d + 2 <= last)(lambda: take_line(d + 2, 0))
        pl.when(early)(lambda: cross(now, 1))
        pl.when((d + 2 <= last) & at_end)(lambda: fill_step(d + 2, 0))
        pl.when((d + 3 <= last) & inner)(lambda: fill_step(d + 3, 0))
        return carry

    lax.fori_loop(0, experts, step_of, 0)

    def weights_of(expert, h):
        names = slots(expert, begin[h], size[h])
        mix = jnp.where(names == target_one, route_ref[0:1, :], 0.0) + jnp.where(
            names == target_two, route_ref[1:2, :], 0.0
        )
        high = mix.astype(jnp.bfloat16)
        return high, (mix - high.astype(jnp.float32)).astype(jnp.bfloat16)

    def combine(expert, h, mixes=None):
        dims = (((0,), (0,)), ((), ()))
        high, low = mixes or weights_of(expert, h)
        values = home[expert, unit(h)]
        return lax.dot_general(
            high, values, dims, preferred_element_type=jnp.float32
        ) + lax.dot_general(low, values, dims, preferred_element_type=jnp.float32)

    def take_home(expert, h):
        mixes = weights_of(expert, h)
        with jax.named_scope("homewait"):
            home_arrival(expert, h).wait_recv()
        total[...] += combine(expert, h, mixes)

    def end_rest():
        for h in range(2):
            cross(at_step(1), h)
        for h in range(2):
            cross(mine, h)
        for step in (last, 1):
            for h in range(2):
                send_home(at_step(step), h)

    def inner_rest():
        for h in range(2):
            cross(mine, h)
        send_home(at_step(last - 1), 1)
        for h in range(2):
            send_home(at_step(last), h)

    pl.when(at_end)(end_rest)
    pl.when(inner)(inner_rest)
    home[mine, unit(0)] = meet(mine, 0)
    total[...] = combine(mine, 0)
    waited = [step for step in range(1, experts) if step != 2] + [2] * (experts > 2)
    for step in waited:
        take_home(at_step(step), 0)
    home[mine, unit(1)] = meet(mine, 1)
    total[...] += combine(mine, 1)
    for step in waited:
        take_home(at_step(step), 1)
    routed = total[...]
    sums[...] = jnp.broadcast_to(
        jnp.sum(routed * routed, axis=1, keepdims=True), (tok_rows, 128)
    ).T[0:8, :]
    sum_copy().start()
    with jax.named_scope("sum1"):
        sum_copy().wait_recv()
    squares_out = sums[...] + peer_sums[...]
    factor_out = lax.rsqrt(squares_out / (2 * width) + norm_eps).T[:, 0:1]
    out_ref[...] = (total[...] * factor_out * gain_out_ref[:, own_cols]).astype(jnp.bfloat16)

    def sent_all(view, sem):
        pltpu.make_async_remote_copy(
            src_ref=view,
            dst_ref=view,
            send_sem=sem,
            recv_sem=sq_recv.at[0],
            device_id={"tp": other},
            device_id_type=MESH,
        ).wait_send()

    others = pl.ds(0, last)
    for side in sides:

        def own_done(side=side):
            sent_all(tok_ref, own_sent.at[(side + 1) // 2])
            own_note(side).wait_send()

        pl.when(is_inner(mine + side))(own_done)
        pl.when(inner & is_end(mine + side))(lambda: sent_all(packed.at[others], sent.at[3]))

    def forwarded(source, carry):
        def done():
            sent_all(notes.at[source], note_sent.at[source])
            sent_all(arrived.at[source], line_sent.at[source])

        up = (source < mine) & is_inner(mine + 1)
        pl.when(inner & (up | ((source > mine) & is_inner(mine - 1))))(done)
        return carry

    lax.fori_loop(0, experts, forwarded, 0)
    sent_all(rows.at[:, :, :, pl.ds(0, width)], sent.at[4])
    sent_all(rows.at[:, 0, :, pl.ds(0, width)], sent.at[5])
    sent_all(parts.at[:, :, pl.ds(0, width)], sent.at[6])
    sent_all(crossing, sent.at[7])
    sent_all(leaving.at[others], sent.at[8])
    square_copy().wait_send()
    sum_copy().wait_send()


def layer(
    tokens, gain_in, gain_out, expert_ids, route_weight, gate_weight, up_weight, down_weight
):
    tok_rows, width = tokens.shape
    experts = lax.axis_size("ep") // 2
    picks = expert_ids.shape[1]
    cap = tok_rows * picks * 3 // (2 * experts)
    hidden_width = gate_weight.shape[2]
    if picks != 2 or experts < 4 or cap % 16 or cap < 32 or width % 256 or hidden_width % 128:
        return plain(
            tokens, gain_in, gain_out, expert_ids, route_weight, gate_weight, up_weight, down_weight
        )
    vmem = pl.BlockSpec(memory_space=pltpu.VMEM)
    hbm = pl.BlockSpec(memory_space=pl.ANY)
    bf16, f32 = jnp.bfloat16, jnp.float32
    dma = pltpu.SemaphoreType.DMA
    return pl.pallas_call(
        functools.partial(fused, experts, cap),
        out_shape=pltpu.VMEM((tok_rows, width), bf16),
        in_specs=[hbm] * 8,
        out_specs=vmem,
        scratch_shapes=[
            pltpu.VMEM((tok_rows, width), bf16),
            pltpu.VMEM((1, 2 * width), f32),
            pltpu.VMEM((1, 2 * width), f32),
            pltpu.VMEM((picks, tok_rows), jnp.int32),
            pltpu.VMEM((picks, tok_rows), f32),
            pltpu.VMEM((experts, tok_rows, width), bf16),
            pltpu.VMEM((experts, 8, tok_rows), f32),
            pltpu.VMEM((experts, cap, width), bf16),
            pltpu.VMEM((experts, 2, cap, 2 * width), bf16),
            pltpu.VMEM((experts, 2 * cap, 2 * width), bf16),
            pltpu.VMEM((experts, 2 * cap, width), bf16),
            pltpu.VMEM((experts, cap, width), bf16),
            pltpu.VMEM((experts, cap, width), bf16),
            pltpu.VMEM((experts, cap, width), bf16),
            pltpu.VMEM((experts, cap, width), bf16),
            pltpu.VMEM((2 * width, 2 * hidden_width), bf16),
            pltpu.VMEM((hidden_width, 2 * width), bf16),
            pltpu.VMEM((8, tok_rows), f32),
            pltpu.VMEM((8, tok_rows), f32),
            pltpu.VMEM((8, tok_rows), f32),
            pltpu.VMEM((8, tok_rows), f32),
            pltpu.VMEM((tok_rows, width), f32),
            dma((2,)),
            dma((5,)),
            dma((9,)),
            dma((4,)),
            dma((experts,)),
            dma((experts,)),
            dma((2,)),
            dma((experts,)),
            dma((2 * experts,)),
            dma((experts,)),
            dma((2 * experts,)),
            dma((2 * experts,)),
            dma((2 * experts,)),
            dma((2 * experts,)),
        ],
        compiler_params=pltpu.CompilerParams(
            collective_id=0, has_side_effects=True, vmem_limit_bytes=60 * 1024 * 1024
        ),
    )(
        tokens,
        gain_in[None, :],
        gain_out[None, :],
        expert_ids.T,
        route_weight.T,
        gate_weight,
        up_weight,
        down_weight,
    )


def solution(mesh):
    in_specs = (
        P(("grp", "ep"), "tp"),
        P(),
        P(),
        P(("grp", "ep"), None),
        P(("grp", "ep"), None),
        P("ep", None, "tp"),
        P("ep", None, "tp"),
        P("ep", "tp", None),
    )
    out_specs = P(("grp", "ep"), "tp")
    return jax.shard_map(layer, mesh=mesh, in_specs=in_specs, out_specs=out_specs, check_vma=False)
```
